32 devices in a mesh: sp: 4 (over z), tp: 4 (over y, x), dp: 2 (over core).
Axes of the slice: x: 2, y: 2, z: 4, core: 2. Of those that a mesh axis runs over, the one named last changes fastest.
Arguments:
- latent: bfloat16 [4, 4096, 2048], P('dp', 'sp'), may hold values from -6 to 6
- context: bfloat16 [4, 1024, 2048], P('dp', 'sp'), may hold values from -6 to 6
- condition: bfloat16 [4, 2048], P('dp', 'sp'), may hold values from -6 to 6
- ctx_cond: bfloat16 [2048], P('sp'), may hold values from -6 to 6
- norm_gain: float32 [2048], replicated, may hold values from 0.1 to 1.9
- w_shift: bfloat16 [2048, 2048], P('sp', 'tp'), may hold values from -0.125 to 0.125
- w_scale: bfloat16 [2048, 2048], P('sp', 'tp'), may hold values from -0.125 to 0.125
- w_gate: bfloat16 [2048, 2048], P('sp', 'tp'), may hold values from -0.125 to 0.125
- w_query: bfloat16 [2048, 1024], P(None, 'tp'), may hold values from -0.125 to 0.125
- w_key: bfloat16 [2048, 256], P(None, 'tp'), may hold values from -0.125 to 0.125
- w_value: bfloat16 [2048, 256], P(None, 'tp'), may hold values from -0.125 to 0.125
- w_out: bfloat16 [1024, 2048], P('tp'), may hold values from -4 to 4
- sink_logit: float32 [16], P('tp'), may hold values from 4 to 7
- ctx_lift: float32 [16], P('tp'), may hold values from -4 to 220
Outputs:
- mixed: bfloat16 [4, 4096, 2048], P('dp', ('sp', 'tp'))
The draws below stay inside these ranges and needn't reach their ends.
All inputs are finite; a program needn't handle non-finite values.
Results may differ from the reference program's by a relative error of at most 0.012.
Values may be sent and summed in bfloat16 or wider, within the bound.
A program may use at most 128 MiB of HBM per device.

```python
import jax
import jax.numpy as jnp
from jax import lax

D = 2048
HEADS = 16
KV_HEADS = 4
HEAD = 64
WINDOW = 128
GRID_COLS = 64
TOK_DEV = 1024
CTX = 1024
SAMPLES = 4
LATENT = 4096


def draw_ctx_lift(key, part):
    first_key = jax.random.fold_in(key, 11)
    lifted = jax.random.uniform(first_key, (HEADS,), jnp.float32, -3.6, -1.8)
    return lifted


def level_of(own_key, dims, cuts, smallest, largest):
    factor_of = 1.0
    for position, blocks in cuts:
        steps = jax.random.uniform(jax.random.fold_in(jax.random.fold_in(own_key, 6), position), (blocks,), jnp.float32, smallest / len(cuts), largest / len(cuts))
        factor_of = factor_of * jnp.repeat(jnp.exp(steps), dims[position] // blocks).reshape((-1,) + (1,) * (len(dims) - 1 - position))
    return factor_of


def centred(stream_key, shape, deviation, limit, cuts=(), kind=jnp.bfloat16):
    level = level_of(stream_key, shape, cuts, -0.22, 0.18) if cuts else 1.0
    array = jax.random.normal(stream_key, shape, jnp.float32) * deviation * level
    return jnp.minimum(jnp.maximum(array, -limit), limit).astype(kind)


def setup_inputs(seed: int = 0) -> dict:
    splits = jax.random.split(jax.random.key(seed), 15)
    return {
        "latent": centred(splits[0], (SAMPLES, LATENT, D), 1.0, 6.0, ((0, 2), (1, 4))),
        "context": centred(splits[1], (SAMPLES, CTX, D), 1.0, 6.0, ((0, 2), (1, 4))),
        "condition": centred(splits[2], (SAMPLES, D), 1.0, 6.0, ((0, 2), (1, 4))),
        "ctx_cond": centred(splits[3], (D,), 1.0, 6.0, ((0, 4),)),
        "norm_gain": jnp.clip(1.0 + 0.18 * jax.random.normal(splits[4], (D,), jnp.float32), 0.1, 1.9),
        "w_shift": centred(splits[5], (D, D), D ** -0.5, 0.125, ((0, 4), (1, 4))),
        "w_scale": centred(splits[6], (D, D), D ** -0.5, 0.125, ((0, 4), (1, 4))),
        "w_gate": centred(splits[7], (D, D), D ** -0.5, 0.125, ((0, 4), (1, 4))),
        "w_query": centred(splits[8], (D, HEADS * HEAD), D ** -0.5, 0.125, ((1, 4),)),
        "w_key": centred(splits[9], (D, KV_HEADS * HEAD), D ** -0.5, 0.125, ((1, 4),)),
        "w_value": centred(splits[10], (D, KV_HEADS * HEAD), D ** -0.5, 0.125, ((1, 4),)),
        "w_out": centred(splits[11], (HEADS * HEAD, D), 2 ** -0.5, 4.0, ((0, 4),)),
        "sink_logit": jnp.clip(4.0 + 3.0 * jax.random.uniform(splits[12], (HEADS,), jnp.float32) ** level_of(splits[12], (HEADS,), ((0, 4),), -0.2, 0.2), 4.0, 7.0),
        "ctx_lift": draw_ctx_lift(jax.random.fold_in(splits[14], 71), 0),
    }


epsilon = 1e-06
rope_base = 10000.0
masked_value = -1e+30

def modulated(inputs, norm_gain, shift_vec, scale_vec):
    widened = inputs.astype(jnp.float32)
    inverse = lax.rsqrt(lax.optimization_barrier(jnp.mean(widened * widened, axis=-1, keepdims=True)) + epsilon)
    return (widened * inverse * norm_gain * (1.0 + scale_vec) + shift_vec).astype(jnp.bfloat16)

def rotate_half(half_part, angles):
    first_half, second = jnp.split(half_part, 2, axis=-1)
    cosine = jnp.cos(angles)[:, None, :]
    sine_part = jnp.sin(angles)[:, None, :]
    return jnp.concatenate([first_half * cosine - second * sine_part, first_half * sine_part + second * cosine], axis=-1)

def rotate(inputs, positions):
    quarter = inputs.shape[-1] // 4
    frequency = rope_base ** (-jnp.arange(quarter, dtype=jnp.float32) / quarter)
    row_angle = (positions // GRID_COLS).astype(jnp.float32)[:, None] * frequency
    col_angle = (positions % GRID_COLS).astype(jnp.float32)[:, None] * frequency
    half_size = 2 * quarter
    return jnp.concatenate([rotate_half(inputs[..., :half_size], row_angle), rotate_half(inputs[..., half_size:], col_angle)], axis=-1)

def reference(latent, context, condition, ctx_cond, norm_gain, w_shift, w_scale, w_gate, w_query, w_key, w_value, w_out, sink_logit, ctx_lift):
    samples, latent_len, model_width = latent.shape
    cond_rows = jnp.concatenate([condition, ctx_cond[None, :]], axis=0)
    active = jax.nn.silu(cond_rows.astype(jnp.float32)).astype(jnp.bfloat16)
    shift_vec = jnp.dot(active, w_shift, preferred_element_type=jnp.float32)
    scale_vec = jnp.dot(active, w_scale, preferred_element_type=jnp.float32)
    gate_vec = jnp.dot(active, w_gate, preferred_element_type=jnp.float32)
    hidden = modulated(latent, norm_gain, shift_vec[:samples, None, :], scale_vec[:samples, None, :])
    ctx_hidden = modulated(context, norm_gain, shift_vec[samples], scale_vec[samples])
    positions = jnp.arange(latent_len, dtype=jnp.int32)
    flat = hidden.reshape(-1, model_width)
    queries = rotate(jnp.dot(flat, w_query, preferred_element_type=jnp.float32).reshape(samples, latent_len, HEADS, HEAD), positions).astype(jnp.bfloat16)
    key_rows = rotate(jnp.dot(flat, w_key, preferred_element_type=jnp.float32).reshape(samples, latent_len, KV_HEADS, HEAD), positions).astype(jnp.bfloat16)
    values = jnp.dot(flat, w_value, preferred_element_type=jnp.float32).astype(jnp.bfloat16).reshape(samples, latent_len, KV_HEADS, HEAD)
    ctx_flat = ctx_hidden.reshape(-1, model_width)
    ctx_keys = jnp.dot(ctx_flat, w_key, preferred_element_type=jnp.float32).astype(jnp.bfloat16).reshape(samples, CTX, KV_HEADS, HEAD)
    ctx_values = jnp.dot(ctx_flat, w_value, preferred_element_type=jnp.float32).astype(jnp.bfloat16).reshape(samples, CTX, KV_HEADS, HEAD)
    padding = ((0, 0), (WINDOW, WINDOW), (0, 0), (0, 0))
    key_pad = jnp.pad(key_rows, padding)
    value_pad = jnp.pad(values, padding)
    block_rows = min(512, TOK_DEV)
    blocks = latent_len // block_rows
    span_rows = block_rows + 2 * WINDOW
    group_size = HEADS // KV_HEADS
    lift_rows = ctx_lift.astype(jnp.float32).reshape(KV_HEADS, group_size, 1, 1)
    sink_rows = sink_logit.astype(jnp.float32).reshape(KV_HEADS, group_size, 1, 1)
    factor = HEAD ** (-0.5)

    def attend(step_id):
        sample = step_id // blocks
        row_start = step_id % blocks * block_rows
        q_rows = lax.dynamic_slice_in_dim(lax.dynamic_index_in_dim(queries, sample, 0, keepdims=False), row_start, block_rows, 0)
        q_rows = q_rows.reshape(block_rows, KV_HEADS, group_size, HEAD).astype(jnp.float32)
        near_keys = lax.dynamic_slice_in_dim(lax.dynamic_index_in_dim(key_pad, sample, 0, keepdims=False), row_start, span_rows, 0).astype(jnp.float32)
        near_values = lax.dynamic_slice_in_dim(lax.dynamic_index_in_dim(value_pad, sample, 0, keepdims=False), row_start, span_rows, 0).astype(jnp.float32)
        far_keys = lax.dynamic_index_in_dim(ctx_keys, sample, 0, keepdims=False).astype(jnp.float32)
        far_values = lax.dynamic_index_in_dim(ctx_values, sample, 0, keepdims=False).astype(jnp.float32)
        query_pos = row_start + jnp.arange(block_rows, dtype=jnp.int32)
        key_pos = row_start - WINDOW + jnp.arange(span_rows, dtype=jnp.int32)
        inside = (key_pos[None, :] >= 0) & (key_pos[None, :] < latent_len) & (jnp.abs(query_pos[:, None] - key_pos[None, :]) <= WINDOW)
        near_scores = jnp.einsum('qgrd,kgd->grqk', q_rows, near_keys) * factor
        near_scores = jnp.where(inside[None, None], near_scores, masked_value)
        far_scores = jnp.einsum('qgrd,kgd->grqk', q_rows, far_keys) * factor + lift_rows
        row_max = jnp.maximum(jnp.maximum(near_scores.max(-1, keepdims=True), far_scores.max(-1, keepdims=True)), sink_rows)
        near_exp = jnp.exp(near_scores - row_max)
        far_exp = jnp.exp(far_scores - row_max)
        normaliser = near_exp.sum(-1, keepdims=True) + far_exp.sum(-1, keepdims=True) + jnp.exp(sink_rows - row_max)
        near_weights = (near_exp / normaliser).astype(jnp.bfloat16).astype(jnp.float32)
        far_weights = (far_exp / normaliser).astype(jnp.bfloat16).astype(jnp.float32)
        outcome = jnp.einsum('grqk,kgd->qgrd', near_weights, near_values) + jnp.einsum('grqk,kgd->qgrd', far_weights, far_values)
        return outcome.astype(jnp.bfloat16).reshape(block_rows, HEADS * HEAD)
    attended = lax.map(attend, jnp.arange(samples * blocks, dtype=jnp.int32)).reshape(samples, latent_len, HEADS * HEAD)
    projected = jnp.dot(attended.reshape(-1, HEADS * HEAD), w_out, preferred_element_type=jnp.float32).reshape(samples, latent_len, model_width)
    return (gate_vec[:samples, None, :] * projected).astype(jnp.bfloat16)
```

```python
import functools

import jax
import jax.numpy as jnp
from jax import lax
from jax.experimental import pallas as pl
from jax.experimental.pallas import tpu as pltpu
from jax.sharding import PartitionSpec as P

HEAD = 64
WINDOW = 128
GRID_COLS = 64
LANES = 128

epsilon = 1e-06
rope_base = 10000.0
masked_value = -1e30
log2e = 1.4426950408889634
MESH = pl.DeviceIdType.MESH


def kernel(
    sizes,
    latent,
    context,
    condition,
    ctx_cond,
    norm_gain,
    w_shift,
    w_scale,
    w_gate,
    w_query,
    w_key,
    w_value,
    w_out,
    sink_logit,
    ctx_lift,
    cosine,
    sine,
    out,
    x_lat,
    x_ctx,
    w_mod,
    w_q,
    w_k,
    w_v,
    w_kv,
    w_o,
    act,
    mod_rx,
    mod_all,
    vec_a,
    vec_b,
    vec_g,
    inv_lat,
    inv_ctx,
    q_buf,
    kv_buf,
    v_buf,
    ckv_buf,
    cv_buf,
    mask_buf,
    att_buf,
    rows_rx,
    ld_sem,
    ma_send,
    ma_recv,
    mb_send,
    mb_recv,
    cx_send,
    cx_recv,
    ha_send,
    ha_recv,
    at_send,
    at_recv,
    wo_send,
    wo_recv,
    wf_send,
    wf_recv,
):
    n_sp, n_tp, n_dp = sizes
    me_sp, me_tp, me_dp = lax.axis_index("sp"), lax.axis_index("tp"), lax.axis_index("dp")
    samples, tokens, width = latent.shape
    ctx_rows = context.shape[1]
    part = w_shift.shape[1]
    heads = w_query.shape[1] // HEAD
    block = tokens // n_tp
    span = block + 2 * WINDOW

    def other(me, step, count):
        return lax.rem(me + step, count)

    barrier = pltpu.get_barrier_semaphore()
    for axis, me, count in (("sp", me_sp, n_sp), ("tp", me_tp, n_tp), ("dp", me_dp, n_dp)):
        for step in range(1, count):
            pl.semaphore_signal(
                barrier, inc=1, device_id={axis: other(me, step, count)}, device_id_type=MESH
            )

    loads = []
    for source, target in (
        (w_shift, w_mod.at[0]),
        (w_scale, w_mod.at[1]),
        (w_gate, w_mod.at[2]),
        (context, x_ctx),
        (latent.at[0], x_lat.at[0]),
        (w_key, w_k),
        (w_value, w_v),
        (w_query, w_q),
        *((latent.at[s], x_lat.at[s]) for s in range(1, samples)),
        (w_out, w_o.at[me_tp]),
    ):
        copy = pltpu.make_async_copy(source, target, ld_sem.at[len(loads)])
        copy.start()
        loads.append(copy)

    act[...] = jnp.zeros_like(act)
    cond = condition[...].astype(jnp.float32)
    act[0:samples, :] = cond / (1.0 + jnp.exp(-cond))
    cond = ctx_cond[...].astype(jnp.float32)
    act[samples : samples + 1, :] = cond / (1.0 + jnp.exp(-cond))
    active = act[...].astype(jnp.bfloat16)
    for i in range(3):
        loads[i].wait()
        mod_rx[me_sp, :, i * part : (i + 1) * part] = jnp.dot(
            active, w_mod[i], preferred_element_type=jnp.float32
        )
    pl.semaphore_wait(barrier, n_sp + n_tp + n_dp - 3)

    def mod_copy(step):
        return pltpu.make_async_remote_copy(
            src_ref=mod_rx.at[me_sp],
            dst_ref=mod_rx.at[me_sp],
            send_sem=ma_send.at[step],
            recv_sem=ma_recv.at[step],
            device_id={"sp": other(me_sp, step, n_sp)},
            device_id_type=MESH,
        )

    for step in range(1, n_sp):
        mod_copy(step).start()

    def inverse_of(rows):
        wide = rows.astype(jnp.float32)
        total = jnp.sum(wide * wide, axis=-1, keepdims=True)
        return jnp.broadcast_to(lax.rsqrt(total / width + epsilon), (rows.shape[0], LANES))

    loads[3].wait()
    for s in range(samples):
        inv_ctx[s] = inverse_of(x_ctx[s])

    def stats(s):
        def body(i, carry):
            rows = pl.ds(pl.multiple_of(i * block, block), block)
            inv_lat[s, rows, :] = inverse_of(x_lat[s, rows, :])
            return carry

        lax.fori_loop(0, n_tp, body, 0)

    loads[4].wait()
    stats(0)
    loads[5].wait()
    loads[6].wait()
    w_kv[...] = jnp.concatenate([w_k[...], w_v[...]], axis=1)

    def wait_mod(step):
        source = other(me_sp, n_sp - step, n_sp)
        pltpu.make_async_remote_copy(
            src_ref=mod_rx.at[source],
            dst_ref=mod_rx.at[source],
            send_sem=ma_send.at[step],
            recv_sem=ma_recv.at[step],
            device_id={"sp": other(me_sp, step, n_sp)},
            device_id_type=MESH,
        ).wait_recv()

    for step in range(1, n_sp):
        wait_mod(step)
    total = mod_rx[0]
    for i in range(1, n_sp):
        total = total + mod_rx[i]
    mod_all[me_tp] = total

    def all_copy(step, source):
        return pltpu.make_async_remote_copy(
            src_ref=mod_all.at[source],
            dst_ref=mod_all.at[source],
            send_sem=mb_send.at[step],
            recv_sem=mb_recv.at[step],
            device_id={"tp": other(me_tp, step, n_tp)},
            device_id_type=MESH,
        )

    for step in range(1, n_tp):
        all_copy(step, me_tp).start()
    for s in range(1, samples):
        loads[7 + s].wait()
        stats(s)
    loads[7].wait()
    for step in range(1, n_tp):
        all_copy(step, other(me_tp, n_tp - step, n_tp)).wait_recv()
    for t in range(n_tp):
        cols = slice(t * part, (t + 1) * part)
        vec_b[:, cols] = mod_all[t, :, 0:part]
        vec_a[:, cols] = (1.0 + mod_all[t, :, part : 2 * part]) * norm_gain[:, cols]
        vec_g[:, cols] = mod_all[t, :, 2 * part : 3 * part]

    share = w_out.shape[0] // n_dp
    mine = pl.ds(pl.multiple_of(me_dp * share, share), share)

    def out_copy(step, source):
        return pltpu.make_async_remote_copy(
            src_ref=w_out.at[mine, :],
            dst_ref=w_o.at[source, mine, :],
            send_sem=wo_send.at[step],
            recv_sem=wo_recv.at[step],
            device_id={"tp": other(me_tp, step, n_tp)},
            device_id_type=MESH,
        )

    def forward_copy(step, hop, part_id):
        source = other(me_tp, n_tp - step, n_tp)
        rows = pl.ds(pl.multiple_of(part_id * share, share), share)
        return pltpu.make_async_remote_copy(
            src_ref=w_o.at[source, rows, :],
            dst_ref=w_o.at[source, rows, :],
            send_sem=wf_send.at[step, hop],
            recv_sem=wf_recv.at[step, hop],
            device_id={"dp": other(me_dp, hop, n_dp)},
            device_id_type=MESH,
        )

    for step in range(1, n_tp):
        out_copy(step, me_tp).start()

    def hidden_of(rows, inverse, row):
        return (
            rows.astype(jnp.float32) * inverse[:, 0:1] * vec_a[row : row + 1, :]
            + vec_b[row : row + 1, :]
        ).astype(jnp.bfloat16)

    def ctx_copy(s, step, source):
        rows = pl.ds(pl.multiple_of(source * ctx_rows, ctx_rows), ctx_rows)
        return pltpu.make_async_remote_copy(
            src_ref=ckv_buf.at[s, rows, :],
            dst_ref=ckv_buf.at[s, rows, :],
            send_sem=cx_send.at[s, step],
            recv_sem=cx_recv.at[s, step],
            device_id={"sp": other(me_sp, step, n_sp)},
            device_id_type=MESH,
        )

    for s in range(samples):
        rows = pl.ds(pl.multiple_of(me_sp * ctx_rows, ctx_rows), ctx_rows)
        ckv_buf[s, rows, :] = jnp.dot(
            hidden_of(x_ctx[s], inv_ctx[s], samples), w_kv[...], preferred_element_type=jnp.float32
        ).astype(jnp.bfloat16)
        for step in range(1, n_sp):
            ctx_copy(s, step, me_sp).start()

    lane = lax.broadcasted_iota(jnp.int32, (block, LANES), 1)
    quarter = HEAD // 4
    first = lane % (2 * quarter) < quarter
    low = lane < HEAD

    def turned(u, cos_rows, sin_rows):
        partner = jnp.where(
            first, pltpu.roll(u, LANES - quarter, 1), pltpu.roll(u, quarter, 1)
        )
        return u * cos_rows + partner * sin_rows

    def project(s):
        def body(i, carry):
            start = pl.multiple_of(i * block, block)
            rows = pl.ds(start, block)
            hid = hidden_of(x_lat[s, rows, :], inv_lat[s, rows, :], s)
            cos_rows, sin_rows = cosine[rows, :], sine[rows, :]
            kv = jnp.dot(hid, w_kv[...], preferred_element_type=jnp.float32)
            kv = jnp.where(low, turned(kv, cos_rows, sin_rows), kv)
            kv_buf[s, pl.ds(pl.multiple_of(start + WINDOW, WINDOW), block), :] = kv.astype(
                jnp.bfloat16
            )
            q = jnp.dot(hid, w_q[...], preferred_element_type=jnp.float32)
            scale = log2e * HEAD ** (-0.5)
            for pair in range(heads // 2):
                u = turned(q[:, pair * LANES : (pair + 1) * LANES], cos_rows, sin_rows) * scale
                q_buf[s, 2 * pair, rows, :] = jnp.where(low, u, 0.0).astype(jnp.bfloat16)
                q_buf[s, 2 * pair + 1, rows, :] = jnp.where(
                    low, pltpu.roll(u, HEAD, 1), 0.0
                ).astype(jnp.bfloat16)
            return carry

        lax.fori_loop(0, n_tp, body, 0)

    def halo_copy(s, side):
        source, target = ((tokens, 0), (WINDOW, WINDOW + tokens))[side]
        step = (1, n_sp - 1)[side]
        return pltpu.make_async_remote_copy(
            src_ref=kv_buf.at[s, pl.ds(source, WINDOW), :],
            dst_ref=kv_buf.at[s, pl.ds(target, WINDOW), :],
            send_sem=ha_send.at[s, side],
            recv_sem=ha_recv.at[s, side],
            device_id={"sp": other(me_sp, step, n_sp)},
            device_id_type=MESH,
        )

    for s in range(samples):
        project(s)
        halo_copy(s, 0).start()
        halo_copy(s, 1).start()

    for s in range(samples):
        for step in range(1, n_sp):
            ctx_copy(s, step, other(me_sp, n_sp - step, n_sp)).wait_recv()
        rows = ckv_buf[s]
        keep = lax.broadcasted_iota(jnp.int32, rows.shape, 1) >= HEAD
        cv_buf[s] = jnp.where(keep, rows.astype(jnp.float32), 1.0).astype(jnp.bfloat16)
    for s in range(samples):
        for side in range(2):
            halo_copy(s, side).wait_recv()
        rows = kv_buf[s]
        keep = lax.broadcasted_iota(jnp.int32, rows.shape, 1) >= HEAD
        v_buf[s] = jnp.where(keep, rows.astype(jnp.float32), 1.0).astype(jnp.bfloat16)

    def rows_copy(s, step, source):
        target = other(me_tp, step, n_tp)
        return pltpu.make_async_remote_copy(
            src_ref=att_buf.at[s, target],
            dst_ref=rows_rx.at[source, s],
            send_sem=at_send.at[s, step],
            recv_sem=at_recv.at[s, step],
            device_id={"tp": target},
            device_id_type=MESH,
        )

    nt = (((1,), (1,)), ((), ()))
    row_id = lax.broadcasted_iota(jnp.int32, (block, span), 0)
    col_id = lax.broadcasted_iota(jnp.int32, (block, span), 1)

    def attend(index, carry):
        s = index // n_tp
        step = index % n_tp + 1
        owner = other(me_tp, step, n_tp)
        start = pl.multiple_of(owner * block, block)
        key_pos = me_sp * tokens + start - WINDOW + col_id
        inside = (
            (key_pos >= 0)
            & (key_pos < n_sp * tokens)
            & (jnp.abs(row_id + WINDOW - col_id) <= WINDOW)
        )
        mask_buf[...] = jnp.where(inside, 0.0, masked_value)
        for h in range(heads):
            q = q_buf[s, h, pl.ds(start, block), :]
            far = lax.dot_general(q, ckv_buf[s], nt, preferred_element_type=jnp.float32)
            near = (
                lax.dot_general(
                    q, kv_buf[s, pl.ds(start, span), :], nt, preferred_element_type=jnp.float32
                )
                + mask_buf[...]
            )
            lift = ctx_lift[h] * log2e
            sink = sink_logit[h] * log2e
            top = jnp.maximum(
                jnp.maximum(
                    jnp.max(near, axis=-1, keepdims=True),
                    jnp.max(far, axis=-1, keepdims=True) + lift,
                ),
                sink,
            )
            near_exp = jnp.exp2(near - top).astype(jnp.bfloat16)
            far_exp = jnp.exp2(far - (top - lift)).astype(jnp.bfloat16)
            both = jnp.dot(
                near_exp, v_buf[s, pl.ds(start, span), :], preferred_element_type=jnp.float32
            ) + jnp.dot(far_exp, cv_buf[s], preferred_element_type=jnp.float32)
            weight = both[:, 0:HEAD] + jnp.exp2(sink - top)
            att_buf[s, owner, :, h * HEAD : (h + 1) * HEAD] = (both[:, HEAD:] / weight).astype(
                jnp.bfloat16
            )

        @pl.when(step < n_tp)
        def _():
            rows_copy(s, step, me_tp).start()

        @pl.when(step == n_tp)
        def _():
            rows_rx[me_tp, s] = att_buf[s, me_tp]

        @pl.when(index == n_tp)
        def _():
            for hop_step in range(1, n_tp):
                out_copy(hop_step, other(me_tp, n_tp - hop_step, n_tp)).wait_recv()
                for hop in range(1, n_dp):
                    forward_copy(hop_step, hop, me_dp).start()

        return carry

    lax.fori_loop(0, samples * n_tp, attend, 0)

    loads[8 + samples - 1].wait()
    for step in range(1, n_tp):
        for hop in range(1, n_dp):
            forward_copy(step, hop, other(me_dp, n_dp - hop, n_dp)).wait_recv()
    chunk = 512
    for s in range(samples):
        for step in range(1, n_tp):
            rows_copy(s, step, other(me_tp, n_tp - step, n_tp)).wait_recv()

        def finish(i, carry):
            cols = pl.ds(pl.multiple_of(i * chunk, chunk), chunk)
            acc = jnp.dot(rows_rx[0, s], w_o[0, :, cols], preferred_element_type=jnp.float32)
            for t in range(1, n_tp):
                acc += jnp.dot(rows_rx[t, s], w_o[t, :, cols], preferred_element_type=jnp.float32)
            out[s, :, cols] = (acc * vec_g[s : s + 1, cols]).astype(jnp.bfloat16)
            return carry

        lax.fori_loop(0, width // chunk, finish, 0)

    for step in range(1, n_sp):
        mod_copy(step).wait_send()
        for s in range(samples):
            ctx_copy(s, step, me_sp).wait_send()
    for s in range(samples):
        halo_copy(s, 0).wait_send()
        halo_copy(s, 1).wait_send()
    for step in range(1, n_tp):
        all_copy(step, me_tp).wait_send()
        out_copy(step, me_tp).wait_send()
        for hop in range(1, n_dp):
            forward_copy(step, hop, me_dp).wait_send()
        for s in range(samples):
            rows_copy(s, step, me_tp).wait_send()


def tables(tokens):
    positions = lax.axis_index("sp") * tokens + jnp.arange(tokens, dtype=jnp.int32)
    lane = jnp.arange(LANES, dtype=jnp.int32)
    quarter = HEAD // 4
    frequency = rope_base ** (-(lane % quarter).astype(jnp.float32) / quarter)
    by_row = lane % HEAD < HEAD // 2
    ticks = jnp.where(by_row, positions[:, None] // GRID_COLS, positions[:, None] % GRID_COLS)
    angles = ticks.astype(jnp.float32) * frequency
    sign = jnp.where(lane % (2 * quarter) < quarter, -1.0, 1.0)
    return jnp.cos(angles), jnp.sin(angles) * sign


def shards(
    latent,
    context,
    condition,
    ctx_cond,
    norm_gain,
    w_shift,
    w_scale,
    w_gate,
    w_query,
    w_key,
    w_value,
    w_out,
    sink_logit,
    ctx_lift,
):
    samples, tokens, width = latent.shape
    ctx_rows = context.shape[1]
    n_sp, n_tp, n_dp = lax.axis_size("sp"), lax.axis_size("tp"), lax.axis_size("dp")
    heads = w_query.shape[1] // HEAD
    assert w_key.shape[1] == HEAD and samples < 8 and heads % 2 == 0
    part = w_shift.shape[1]
    block = tokens // n_tp
    cosine, sine = tables(tokens)
    bf16, f32 = jnp.bfloat16, jnp.float32
    vmem = pl.BlockSpec(memory_space=pltpu.VMEM)
    smem = pl.BlockSpec(memory_space=pltpu.SMEM)
    anywhere = pl.BlockSpec(memory_space=pl.ANY)
    dma = pltpu.SemaphoreType.DMA
    padded = tokens + 2 * WINDOW
    return pl.pallas_call(
        functools.partial(kernel, (n_sp, n_tp, n_dp)),
        out_shape=jax.ShapeDtypeStruct((samples, block, width), bf16),
        in_specs=[
            anywhere,
            anywhere,
            vmem,
            vmem,
            vmem,
            anywhere,
            anywhere,
            anywhere,
            anywhere,
            anywhere,
            anywhere,
            anywhere,
            smem,
            smem,
            vmem,
            vmem,
        ],
        out_specs=vmem,
        scratch_shapes=[
            pltpu.VMEM(latent.shape, bf16),
            pltpu.VMEM(context.shape, bf16),
            pltpu.VMEM((3,) + w_shift.shape, bf16),
            pltpu.VMEM(w_query.shape, bf16),
            pltpu.VMEM(w_key.shape, bf16),
            pltpu.VMEM(w_value.shape, bf16),
            pltpu.VMEM((width, 2 * HEAD), bf16),
            pltpu.VMEM((n_tp,) + w_out.shape, bf16),
            pltpu.VMEM((8, w_shift.shape[0]), f32),
            pltpu.VMEM((n_sp, 8, 3 * part), f32),
            pltpu.VMEM((n_tp, 8, 3 * part), f32),
            pltpu.VMEM((8, width), f32),
            pltpu.VMEM((8, width), f32),
            pltpu.VMEM((8, width), f32),
            pltpu.VMEM((samples, tokens, LANES), f32),
            pltpu.VMEM((samples, ctx_rows, LANES), f32),
            pltpu.VMEM((samples, heads, tokens, LANES), bf16),
            pltpu.VMEM((samples, padded, LANES), bf16),
            pltpu.VMEM((samples, padded, LANES), bf16),
            pltpu.VMEM((samples, n_sp * ctx_rows, LANES), bf16),
            pltpu.VMEM((samples, n_sp * ctx_rows, LANES), bf16),
            pltpu.VMEM((block, block + 2 * WINDOW), f32),
            pltpu.VMEM((samples, n_tp, block, heads * HEAD), bf16),
            pltpu.VMEM((n_tp, samples, block, heads * HEAD), bf16),
            dma((8 + samples,)),
            dma((n_sp,)),
            dma((n_sp,)),
            dma((n_tp,)),
            dma((n_tp,)),
            dma((samples, n_sp)),
            dma((samples, n_sp)),
            dma((samples, 2)),
            dma((samples, 2)),
            dma((samples, n_tp)),
            dma((samples, n_tp)),
            dma((n_tp,)),
            dma((n_tp,)),
            dma((n_tp, n_dp)),
            dma((n_tp, n_dp)),
        ],
        compiler_params=pltpu.CompilerParams(
            collective_id=0, has_side_effects=True, vmem_limit_bytes=60 * 1024 * 1024
        ),
    )(
        latent,
        context,
        condition,
        ctx_cond.reshape(1, -1),
        norm_gain.reshape(1, -1),
        w_shift,
        w_scale,
        w_gate,
        w_query,
        w_key,
        w_value,
        w_out,
        sink_logit,
        ctx_lift,
        cosine,
        sine,
    )


def solution(mesh):
    return jax.shard_map(
        shards,
        mesh=mesh,
        in_specs=(
            P("dp", "sp", None),
            P("dp", "sp", None),
            P("dp", "sp"),
            P("sp"),
            P(),
            P("sp", "tp"),
            P("sp", "tp"),
            P("sp", "tp"),
            P(None, "tp"),
            P(None, "tp"),
            P(None, "tp"),
            P("tp", None),
            P("tp"),
            P("tp"),
        ),
        out_specs=P("dp", ("sp", "tp"), None),
        check_vma=False,
    )
```
